32 devices in a mesh: ep: 8 (over z, x), tp: 4 (over y, core).
Axes of the slice: x: 2, y: 2, z: 4, core: 2. Of those that a mesh axis runs over, the one named last changes fastest.
Arguments:
- tokens: bfloat16 [4608, 2048], P(('ep', 'tp')), may hold values from -6 to 6
- norm_gain: float32 [2048], replicated, may hold values from 0.1 to 1.9
- expert_ids: int32 [4608, 8], P(('ep', 'tp')), may hold values from 0 to 15, all different within a row; in each aligned block of 144 rows (0 to 143, 144 to 287, ...) at most 144 rows name the same one
- route_weights: float32 [4608, 8], P(('ep', 'tp')), may hold values from 0.3 to 1
- expert_gate: bfloat16 [16, 512, 2048], P('ep', 'tp'), may hold values from -0.125 to 0.125
- expert_up: bfloat16 [16, 512, 2048], P('ep', 'tp'), may hold values from -0.125 to 0.125
- expert_down: bfloat16 [16, 512, 2048], P('ep', 'tp'), may hold values from -0.25 to 0.25
- shared_gate: bfloat16 [512, 2048], P('tp'), may hold values from -0.125 to 0.125
- shared_up: bfloat16 [512, 2048], P('tp'), may hold values from -0.125 to 0.125
- shared_down: bfloat16 [512, 2048], P('tp'), may hold values from -0.25 to 0.25
- side_in: bfloat16 [2048, 1024], P('ep'), may hold values from -0.125 to 0.125
- side_out: bfloat16 [2048, 1024], P('ep'), may hold values from -0.1875 to 0.1875
- side_gate: bfloat16 [2048], replicated, may hold values from -0.125 to 0.125
Outputs:
- mixed: bfloat16 [4608, 2048], P(('ep', 'tp'))
The draws below stay inside these ranges and needn't reach their ends.
Inputs may be any that keep to these rules, and one draw needn't show every extreme that they name: `expert_ids`: each row names 8 different experts of 0 to 15; within the rows of one device (aligned blocks of 144 rows) no expert is named more than 144 times, and in some of those blocks some expert is named exactly 144 times.
All inputs are finite; a program needn't handle non-finite values.
Results may differ from the reference program's by a relative error of at most 0.0068.
Values may be sent and summed in bfloat16 or wider, within the bound.
A program may use at most 320 MiB of HBM per device.

```python
import math
import jax
import jax.numpy as jnp
import numpy as np
from jax import lax

D = 2048
FF = 512
SIDE = 1024
TOP = 8
TOK_DEV = 144
EXPERTS = 16
CAP = 144
TOKENS = 4608


def levels(stream_key, extent, pieces, smallest, largest):
    level = 1.0
    for dim, blocks in pieces:
        steps = jax.random.uniform(jax.random.fold_in(jax.random.fold_in(stream_key, 6), dim), (blocks,), jnp.float32, smallest / len(pieces), largest / len(pieces))
        level = level * jnp.repeat(jnp.exp(steps), extent[dim] // blocks).reshape((-1,) + (1,) * (len(extent) - 1 - dim))
    return level


def shared_out(rng, own, number, rows, number_of, top, bound, skew):
    ranking = jax.random.permutation(rng, number_of)
    heavy_load, common = portions_of(number_of, rows * top, bound, skew, True), portions_of(number_of, rows * top, bound, skew, False)
    places = jnp.arange(number_of)

    def named(lengths, rotation):
        used = int((lengths > 0).sum())
        fixed = max(1, used // 4)
        shifted = fixed + (places - fixed + rotation * (used - fixed)) % max(1, number_of - fixed)
        return jnp.zeros((number_of,), jnp.int32).at[ranking[jnp.where(places < fixed, places, shifted)]].set(jnp.asarray(lengths, jnp.int32))

    lengths = jnp.where(number % 4 == 0, named(heavy_load, number // 4), named(common, number - number // 4 - 1))
    mixed = jax.random.permutation(jax.random.fold_in(own, 3), number_of)
    source_of, receiver = mixed[0:number_of // 2 * 2:2], mixed[1:number_of // 2 * 2:2]
    slack = jnp.minimum(lengths[source_of] - 1, bound - lengths[receiver]) // 2
    slack = jnp.where((source_of == ranking[0]) | (receiver == ranking[0]) | (lengths[receiver] == 0), 0, jnp.maximum(slack, 0))
    shifted = jax.random.randint(jax.random.fold_in(own, 4), (number_of // 2,), 0, 1 << 20) % (slack + 1)
    lengths = lengths.at[source_of].add(-shifted).at[receiver].add(shifted)
    items = jnp.searchsorted(jnp.cumsum(lengths), jnp.arange(rows * top), side="right").astype(jnp.int32)
    listing = items.reshape(top, rows).T
    listing = listing[jax.random.permutation(jax.random.fold_in(own, 1), rows)]
    rotation = jax.random.randint(jax.random.fold_in(own, 2), (rows, 1), 0, top)
    return jnp.take_along_axis(listing, (jnp.arange(top)[None, :] + rotation) % top, axis=1)


def portions_of(amount, total, reach, slope, full):
    loads = [(1 << 20) // math.isqrt(rank ** slope) + 1 for rank in range(1, amount + 1)]
    largest = reach if full else min(reach, max(-(-total // amount), total * loads[0] // sum(loads)))
    least = 1 if total - largest >= amount - 1 else 0
    holding, spare = [largest] + [least] * (amount - 1), total - largest - least * (amount - 1)
    while spare > 0:
        free = [i for i in range(1, amount) if holding[i] < largest] or [i for i in range(1, amount) if holding[i] < reach]
        pool, left = sum([loads[i] for i in free]), spare
        for i in free:
            addition = min(reach - holding[i], max(1, left * loads[i] // pool), spare)
            holding[i] = holding[i] + addition
            spare = spare - addition
    return np.array(holding)


def centred(key, dims, scale, reach, split=(), kind=jnp.bfloat16):
    gain = levels(key, dims, split, -0.22, 0.18) if split else 1.0
    array = jax.random.normal(key, dims, jnp.float32) * scale * gain
    return jnp.minimum(jnp.maximum(array, -reach), reach).astype(kind)


def setup_inputs(seed: int = 0) -> dict:
    arg_keys = jax.random.split(jax.random.key(seed), 14)
    tokens = centred(arg_keys[0], (TOKENS, D), 1.0, 6.0, ((0, 32),))
    norm_gain = jnp.clip(1.0 + 0.18 * jax.random.normal(arg_keys[1], (D,), jnp.float32), 0.1, 1.9)
    expert_ids_keys = jax.random.split(jax.random.fold_in(arg_keys[2], 1), TOKENS // TOK_DEV)
    expert_ids_turns = jax.random.permutation(jax.random.fold_in(arg_keys[2], 3), TOKENS // TOK_DEV)
    expert_ids = jax.vmap(lambda own, number: shared_out(jax.random.fold_in(arg_keys[2], 2), own, number, TOK_DEV, EXPERTS, TOP, CAP, 2))(expert_ids_keys, expert_ids_turns).reshape((TOKENS, TOP))
    route_weights = jnp.clip(0.3 + 0.7 * jax.random.uniform(arg_keys[3], (TOKENS, TOP), jnp.float32) ** levels(arg_keys[3], (TOKENS, TOP), ((0, 32),), -0.2, 0.2), 0.3, 1.0)
    expert_gate = centred(arg_keys[4], (EXPERTS, FF, D), D ** -0.5, 0.125, ((0, 8), (1, 4)))
    expert_up = centred(arg_keys[5], (EXPERTS, FF, D), D ** -0.5, 0.125, ((0, 8), (1, 4)))
    expert_down = centred(arg_keys[6], (EXPERTS, FF, D), FF ** -0.5, 0.25, ((0, 8), (1, 4)))
    shared_gate = centred(arg_keys[7], (FF, D), D ** -0.5, 0.125, ((0, 4),))
    shared_up = centred(arg_keys[8], (FF, D), D ** -0.5, 0.125, ((0, 4),))
    shared_down = centred(arg_keys[9], (FF, D), FF ** -0.5, 0.25, ((0, 4),))
    side_in = centred(arg_keys[10], (D, SIDE), D ** -0.5, 0.125, ((0, 8),))
    side_out = centred(arg_keys[11], (D, SIDE), SIDE ** -0.5, 0.1875, ((0, 8),))
    side_gate = centred(arg_keys[12], (D,), D ** -0.5, 0.125)
    return dict(tokens=tokens, norm_gain=norm_gain, expert_ids=expert_ids, route_weights=route_weights, expert_gate=expert_gate, expert_up=expert_up, expert_down=expert_down, shared_gate=shared_gate, shared_up=shared_up, shared_down=shared_down, side_in=side_in, side_out=side_out, side_gate=side_gate)


norm_eps = 1.0
row_block = 512

def normalize(tokens, norm_gain):
    values = tokens.astype(jnp.float32)
    scale_inv = lax.rsqrt(lax.optimization_barrier(jnp.mean(values * values, axis=-1, keepdims=True)) + norm_eps)
    return (values * scale_inv * norm_gain).astype(jnp.bfloat16)

def swiglu(gate_part, up_part):
    return (jax.nn.silu(gate_part) * up_part).astype(jnp.bfloat16)

def reference(tokens, norm_gain, expert_ids, route_weights, expert_gate, expert_up, expert_down, shared_gate, shared_up, shared_down, side_in, side_out, side_gate):
    normed = normalize(tokens, norm_gain)
    pair_count = TOKENS * TOP
    flat_ids = expert_ids.reshape(pair_count).astype(jnp.int32)
    flat_tokens = (jnp.arange(pair_count, dtype=jnp.int32) // TOP).astype(jnp.int32)
    flat_weights = route_weights.reshape(pair_count)
    order = jnp.argsort(flat_ids, stable=True)
    sorted_ids = flat_ids[order]
    counts = jnp.bincount(flat_ids, length=EXPERTS).astype(jnp.int32)
    starts = (jnp.cumsum(counts) - counts).astype(jnp.int32)
    padded = ((counts + row_block - 1) // row_block * row_block).astype(jnp.int32)
    ends = jnp.cumsum(padded).astype(jnp.int32)
    begins = (ends - padded).astype(jnp.int32)
    target = (begins[sorted_ids] + jnp.arange(pair_count, dtype=jnp.int32) - starts[sorted_ids]).astype(jnp.int32)
    block_count = (pair_count + EXPERTS * (row_block - 1)) // row_block + 1
    slots_all = block_count * row_block
    token_slots = jnp.full((slots_all,), TOKENS, jnp.int32).at[target].set(flat_tokens[order])
    weight_slots = jnp.zeros((slots_all,), jnp.float32).at[target].set(flat_weights[order])
    block_starts = (jnp.arange(block_count, dtype=jnp.int32) * row_block).astype(jnp.int32)
    block_expert = jnp.minimum(jnp.searchsorted(ends, block_starts, side='right'), EXPERTS - 1).astype(jnp.int32)
    extended = jnp.concatenate([normed, jnp.zeros((1, D), normed.dtype)], axis=0)

    def block_step(running, inputs):
        slot_tokens, slot_weights, expert = inputs
        chosen = extended[slot_tokens]
        gate_part = jnp.dot(chosen, expert_gate[expert].T, preferred_element_type=jnp.float32)
        up_part = jnp.dot(chosen, expert_up[expert].T, preferred_element_type=jnp.float32)
        hidden = swiglu(gate_part, up_part)
        output = jnp.dot(hidden, expert_down[expert], preferred_element_type=jnp.float32).astype(jnp.bfloat16)
        output = lax.optimization_barrier(output).astype(jnp.float32)
        return (running.at[slot_tokens].add(output * slot_weights[:, None]), None)
    running = jnp.zeros((TOKENS + 1, D), jnp.float32)
    running, unused = lax.scan(block_step, running, (token_slots.reshape(block_count, row_block), weight_slots.reshape(block_count, row_block), block_expert))
    routed = running[:TOKENS]
    shared_hidden = swiglu(jnp.dot(normed, shared_gate.T, preferred_element_type=jnp.float32), jnp.dot(normed, shared_up.T, preferred_element_type=jnp.float32))
    shared = jnp.dot(shared_hidden, shared_down, preferred_element_type=jnp.float32)
    side_hidden = jax.nn.silu(jnp.dot(normed, side_in, preferred_element_type=jnp.float32)).astype(jnp.bfloat16)
    side_value = jnp.dot(side_hidden, side_out.T, preferred_element_type=jnp.float32)
    opening = jax.nn.sigmoid(jnp.dot(normed, side_gate, preferred_element_type=jnp.float32))
    return (routed + shared + opening[:, None] * side_value).astype(jnp.bfloat16)
```

```python
import jax
import jax.numpy as jnp
from jax import lax
from jax.sharding import PartitionSpec as P

norm_eps = 1.0


def normalize(tokens, norm_gain):
    values = tokens.astype(jnp.float32)
    scale_inv = lax.rsqrt(jnp.mean(values * values, axis=-1, keepdims=True) + norm_eps)
    return (values * scale_inv * norm_gain).astype(jnp.bfloat16)


def body(
    tokens,
    norm_gain,
    expert_ids,
    route_weights,
    expert_gate,
    expert_up,
    expert_down,
    shared_gate,
    shared_up,
    shared_down,
    side_in,
    side_out,
    side_gate,
):
    normed = normalize(tokens, norm_gain)
    tok_count, width = normed.shape
    groups = lax.axis_size("ep")
    me = lax.axis_index("ep")
    local_experts, ff_part, _ = expert_gate.shape
    experts_all = groups * local_experts
    shared_rows = shared_gate.shape[0] // groups
    side_all = side_in.shape[1]
    side_cols = side_all // groups

    named = expert_ids[:, :, None] == jnp.arange(experts_all, dtype=jnp.int32)
    dense = jnp.sum(jnp.where(named, route_weights[:, :, None], 0.0), axis=1)
    opening = jax.nn.sigmoid(jnp.dot(normed, side_gate, preferred_element_type=jnp.float32))
    aux = jnp.concatenate([dense, opening[:, None]], axis=1)

    all_normed = lax.all_gather(normed, "ep", axis=0, tiled=True)
    all_aux = lax.all_gather(aux, "ep", axis=0, tiled=True)

    def pack(expert_part, shared_part):
        own = lax.dynamic_slice_in_dim(shared_part, me * shared_rows, shared_rows, 0)
        return jnp.concatenate([expert_part.reshape(local_experts * ff_part, width), own], axis=0)

    gate_all = lax.all_gather(pack(expert_gate, shared_gate), "tp", axis=0, tiled=True)
    up_all = lax.all_gather(pack(expert_up, shared_up), "tp", axis=0, tiled=True)
    down_all = lax.all_gather(pack(expert_down, shared_down), "tp", axis=0, tiled=True)

    rows = side_in.shape[0]
    both = jnp.stack([side_in, side_out]).reshape(2, rows, groups, side_cols)
    both = lax.all_to_all(both.transpose(2, 0, 1, 3), "ep", split_axis=0, concat_axis=0, tiled=True)
    in_part = both[:, 0].reshape(groups * rows, side_cols)
    out_part = both[:, 1].reshape(groups * rows, side_cols)

    mine = lax.dynamic_slice_in_dim(all_aux, me * local_experts, local_experts, 1)
    block = local_experts * ff_part + shared_rows
    place = jnp.arange(gate_all.shape[0], dtype=jnp.int32) % block // ff_part
    scale = jnp.ones((all_normed.shape[0], gate_all.shape[0]), jnp.float32)
    for e in range(local_experts):
        scale = jnp.where(place[None, :] == e, mine[:, e : e + 1], scale)

    gate_part = jnp.einsum("td,fd->tf", all_normed, gate_all, preferred_element_type=jnp.float32)
    up_part = jnp.einsum("td,fd->tf", all_normed, up_all, preferred_element_type=jnp.float32)
    hidden = (jax.nn.silu(gate_part) * up_part * scale).astype(jnp.bfloat16)
    side_hidden = jax.nn.silu(jnp.dot(all_normed, in_part, preferred_element_type=jnp.float32))
    side_hidden = (side_hidden * all_aux[:, experts_all:]).astype(jnp.bfloat16)
    total = jnp.dot(hidden, down_all, preferred_element_type=jnp.float32)
    total = total + jnp.einsum("ts,ds->td", side_hidden, out_part, preferred_element_type=jnp.float32)
    return lax.psum_scatter(total.astype(jnp.bfloat16), "ep", scatter_dimension=0, tiled=True)


def solution(mesh):
    placed = (
        P(("ep", "tp"), None),
        P(),
        P(("ep", "tp"), None),
        P(("ep", "tp"), None),
        P("ep", "tp", None),
        P("ep", "tp", None),
        P("ep", "tp", None),
        P("tp", None),
        P("tp", None),
        P("tp", None),
        P("ep", None),
        P("ep", None),
        P(),
    )
    return jax.shard_map(
        body, mesh=mesh, in_specs=placed, out_specs=P(("ep", "tp"), None), check_vma=False
    )
```

```python
import functools

import jax
import jax.numpy as jnp
from jax import lax
from jax.experimental import pallas as pl
from jax.experimental.pallas import tpu as pltpu
from jax.sharding import PartitionSpec as P

norm_eps = 1.0
MESH = pl.DeviceIdType.MESH
NT = (((1,), (1,)), ((), ()))


def normalize(tokens, norm_gain):
    values = tokens.astype(jnp.float32)
    scale_inv = lax.rsqrt(jnp.mean(values * values, axis=-1, keepdims=True) + norm_eps)
    return (values * scale_inv * norm_gain).astype(jnp.bfloat16)


def silu(v):
    return v / (1.0 + jnp.exp(-v))


def kernel(
    dims,
    payload_ref, gate_ref, up_ref, down_ref, side_ref, mask_ref,
    out_ref,
    tok, wg, wu, wd, side, hidden, side_hid, acc, xs, xr, sent, got,
    tok_send, tok_recv, w_send, w_recv, side_send, side_recv,
    x_send, x_recv, r_send, r_recv, l_send, l_recv,
):
    nz, nx, ny, nc, experts_all, local_experts, chunks = dims
    n_ep, n_tp = nz * nx, ny * nc
    me, tp = lax.axis_index("ep"), lax.axis_index("tp")
    z, x = me // nx, me % nx
    y, c = tp // nc, tp % nc
    rows = payload_ref.shape[0]
    width = out_ref.shape[1]
    part = gate_ref.shape[0]
    piece = width // chunks
    side_rows = side_ref.shape[2]

    def cols(q):
        return pl.ds(pl.multiple_of(q * piece, piece), piece)

    barrier = pltpu.get_barrier_semaphore()
    for j in range(1, n_ep):
        pl.semaphore_signal(barrier, inc=1, device_id=((me + j) % n_ep, tp), device_id_type=MESH)
    for j in range(1, n_tp):
        pl.semaphore_signal(barrier, inc=1, device_id=(me, (tp + j) % n_tp), device_id_type=MESH)
    pl.semaphore_wait(barrier, n_ep + n_tp - 2)

    def tok_rows(bz, bx):
        return pl.ds(pl.multiple_of((bx * nz + bz) * rows, rows), rows)

    def tok_copy(bz, way, own):
        if way < 2:
            target = (me + nx if way == 0 else me - nx, tp)
        else:
            target = (z * nx + (x + way - 1) % nx, tp)
        return pltpu.make_async_remote_copy(
            src_ref=payload_ref if own else tok.at[tok_rows(bz, x)],
            dst_ref=tok.at[tok_rows(bz, x)],
            send_sem=tok_send.at[bz, way],
            recv_sem=tok_recv.at[x * nz + bz],
            device_id=target,
            device_id_type=MESH,
        )

    def tok_wait(bz, bx):
        pltpu.make_async_remote_copy(
            src_ref=payload_ref,
            dst_ref=tok.at[tok_rows(bz, bx)],
            send_sem=tok_send.at[0, 0],
            recv_sem=tok_recv.at[bx * nz + bz],
            device_id=(me, tp),
            device_id_type=MESH,
        ).wait_recv()

    def w_refs(k, owner, own):
        if k == 0:
            return (gate_ref if own else wg.at[owner]), wg.at[owner]
        if k == 1:
            return (up_ref if own else wu.at[owner]), wu.at[owner]
        q = cols(k - 2)
        return (down_ref.at[:, q] if own else wd.at[owner, :, q]), wd.at[owner, :, q]

    def w_copy(k, by, way, own):
        if way < 2:
            target = (me, tp + nc if way == 0 else tp - nc)
        else:
            target = (me, y * nc + (c + way - 1) % nc)
        owner = by * nc + c
        src, dst = w_refs(k, owner, own)
        return pltpu.make_async_remote_copy(
            src_ref=src,
            dst_ref=dst,
            send_sem=w_send.at[k, by, way],
            recv_sem=w_recv.at[k, owner],
            device_id=target,
            device_id_type=MESH,
        )

    def w_wait(k, owner):
        src, dst = w_refs(k, owner, True)
        pltpu.make_async_remote_copy(
            src_ref=src, dst_ref=dst, send_sem=w_send.at[0, 0, 0], recv_sem=w_recv.at[k, owner],
            device_id=(me, tp), device_id_type=MESH,
        ).wait_recv()

    def side_copy(j):
        to = (me + j) % n_ep
        return pltpu.make_async_remote_copy(
            src_ref=side_ref.at[to],
            dst_ref=side.at[me],
            send_sem=side_send.at[j],
            recv_sem=side_recv.at[me],
            device_id=(to, tp),
            device_id_type=MESH,
        )

    def each_own(copy_of, at, last, ways, act):
        @pl.when(at < last)
        def _():
            act(copy_of(0))

        @pl.when(at > 0)
        def _():
            act(copy_of(1))

        for way in range(2, ways):
            act(copy_of(way))

    def each_forward(copy_of, index_of, at, last, ways, step, act, arrive):
        @pl.when(at >= step)
        def _():
            b = at - step
            arrive(b)

            @pl.when(at < last)
            def _():
                act(copy_of(b, 0))

            for way in range(2, ways):
                act(copy_of(b, way))

        @pl.when(at + step <= last)
        def _():
            b = at + step
            arrive(b)

            @pl.when(at > 0)
            def _():
                act(copy_of(b, 1))

            for way in range(2, ways):
                act(copy_of(b, way))

    start = lambda copy: copy.start()
    finish = lambda copy: copy.wait_send()
    nothing = lambda b: None
    tok_ways, w_ways = 1 + nx, 1 + nc
    pieces = 2 + chunks

    def tok_forward(step, act, arrive):
        each_forward(
            lambda b, way: tok_copy(b, way, False), None, z, nz - 1, tok_ways, step, act, arrive
        )

    def w_forward(k, step, act, arrive):
        each_forward(
            lambda b, way: w_copy(k, b, way, False), None, y, ny - 1, w_ways, step, act, arrive
        )

    def w_gathered(k):
        for step in range(1, ny):
            w_forward(k, step, start, lambda b: w_wait(k, b * nc + c))

    def w_across(k):
        for j in range(1, nc):
            for by in range(ny):
                w_wait(k, by * nc + (c + j) % nc)

    each_own(lambda way: tok_copy(z, way, True), z, nz - 1, tok_ways, start)
    for k in range(pieces):
        each_own(lambda way: w_copy(k, y, way, True), y, ny - 1, w_ways, start)
    for j in range(1, n_ep):
        side_copy(j).start()
    tok[tok_rows(z, x)] = payload_ref[...]
    wg[tp] = gate_ref[...]
    wu[tp] = up_ref[...]
    wd[tp] = down_ref[...]
    side[me] = side_ref[me]

    def arrive_tok(b):
        tok_wait(b, x)

    for step in range(1, nz):
        tok_forward(step, start, arrive_tok)
        if step == nz - 2:
            w_gathered(0)
    w_gathered(1)
    w_across(0)
    w_across(1)
    for j in range(1, n_ep):
        b = (me + j) % n_ep
        pltpu.make_async_remote_copy(
            src_ref=side_ref.at[b], dst_ref=side.at[b], send_sem=side_send.at[0],
            recv_sem=side_recv.at[b], device_id=(me, tp), device_id_type=MESH,
        ).wait_recv()

    tile = 2 * rows
    for j in range(nx):
        bx = (x + j) % nx
        if j:
            for bz in range(nz):
                tok_wait(bz, bx)

        def hidden_tile(i, carry):
            at = pl.ds(pl.multiple_of(bx * nz * rows + i * tile, rows), tile)
            a = tok[at, :width]
            gate_part = lax.dot_general(
                a, wg[...].reshape(n_tp * part, width), NT, preferred_element_type=jnp.float32
            )
            up_part = lax.dot_general(
                a, wu[...].reshape(n_tp * part, width), NT, preferred_element_type=jnp.float32
            )
            aux = tok[at, width:].astype(jnp.float32)
            lane = lax.broadcasted_iota(jnp.int32, aux.shape, 1)

            def column(n):
                hit = jnp.logical_or(lane == n, lane == n + 64)
                return jnp.sum(jnp.where(hit, aux, 0.0), axis=1, keepdims=True)

            scale = mask_ref[local_experts : local_experts + 1, :]
            for e in range(local_experts):
                scale = scale + column(me * local_experts + e) * mask_ref[e : e + 1, :]
            hidden[at] = (silu(gate_part) * up_part * scale).astype(jnp.bfloat16)
            side_part = jnp.dot(
                a, side[:, 0].reshape(width, side.shape[3]), preferred_element_type=jnp.float32
            )
            side_hid[at] = (silu(side_part) * column(experts_all)).astype(jnp.bfloat16)
            return carry

        lax.fori_loop(0, nz * rows // tile, hidden_tile, 0)

    def x_copy(q, j, bz):
        block = pl.ds(bz * rows, rows)
        return pltpu.make_async_remote_copy(
            src_ref=xs.at[q, j - 1, block],
            dst_ref=xr.at[q, j - 1, block],
            send_sem=x_send.at[q, j - 1, bz],
            recv_sem=x_recv.at[q, j - 1, bz],
            device_id=(z * nx + (x + j) % nx, tp),
            device_id_type=MESH,
        )

    def r_copy(q, dz):
        return pltpu.make_async_remote_copy(
            src_ref=sent.at[q, dz], dst_ref=got.at[q, dz + 1], send_sem=r_send.at[q, dz],
            recv_sem=r_recv.at[q, dz], device_id=(me + nx, tp), device_id_type=MESH,
        )

    def l_copy(q, dz):
        return pltpu.make_async_remote_copy(
            src_ref=sent.at[q, dz], dst_ref=got.at[q, dz], send_sem=l_send.at[q, dz],
            recv_sem=l_recv.at[q, dz], device_id=(me - nx, tp), device_id_type=MESH,
        )

    blocks_per = piece // side_rows

    def multiply(q):
        down = wd[:, :, cols(q)].reshape(n_tp * part, piece)
        side_down = side[pl.ds(q * blocks_per, blocks_per), 1].reshape(piece, side.shape[3])
        for j in list(range(1, nx)) + [0]:
            at = pl.ds(pl.multiple_of((x + j) % nx * nz * rows, rows), nz * rows)
            value = jnp.dot(hidden[at], down, preferred_element_type=jnp.float32)
            value = value + lax.dot_general(
                side_hid[at], side_down, NT, preferred_element_type=jnp.float32
            )
            if j:
                xs[q, j - 1] = value.astype(jnp.bfloat16)
                for bz in range(nz):
                    x_copy(q, j, bz).start()
            else:
                acc[q] = value

    def reduce(q):
        def own(dz):
            block = pl.ds(pl.multiple_of(dz * rows, rows), rows)
            value = acc[q, block]
            for j in range(1, nx):
                x_copy(q, j, dz).wait_recv()
                value = value + xr[q, j - 1, block].astype(jnp.float32)
            return value

        def right(dz):
            value = own(dz)

            @pl.when(z == 0)
            def _():
                sent[q, dz] = value.astype(jnp.bfloat16)

            @pl.when(z > 0)
            def _():
                r_copy(q, dz).wait_recv()
                sent[q, dz] = (value + got[q, dz + 1].astype(jnp.float32)).astype(jnp.bfloat16)

            r_copy(q, dz).start()

        def left(dz):
            value = own(dz)

            @pl.when(z == nz - 1)
            def _():
                sent[q, dz] = value.astype(jnp.bfloat16)

            @pl.when(z < nz - 1)
            def _():
                l_copy(q, dz).wait_recv()
                sent[q, dz] = (value + got[q, dz].astype(jnp.float32)).astype(jnp.bfloat16)

            l_copy(q, dz).start()

        for k in range(nz - 1):
            pl.when(z < nz - 1 - k)(functools.partial(right, nz - 1 - k))
            pl.when(z > k)(functools.partial(left, k))
        acc[q, pl.ds(0, rows)] = own(z)

    def settle(q):
        @pl.when(z > 0)
        def _():
            r_copy(q, z).wait_recv()
            acc[q, pl.ds(0, rows)] += got[q, z + 1].astype(jnp.float32)

        @pl.when(z < nz - 1)
        def _():
            l_copy(q, z).wait_recv()
            acc[q, pl.ds(0, rows)] += got[q, z].astype(jnp.float32)

        out_ref[:, cols(q)] = acc[q, pl.ds(0, rows)].astype(jnp.bfloat16)

    for q in range(chunks):
        w_gathered(2 + q)
        w_across(2 + q)
        multiply(q)
        if q:
            reduce(q - 1)
    reduce(chunks - 1)
    for q in range(chunks):
        settle(q)

    each_own(lambda way: tok_copy(z, way, True), z, nz - 1, tok_ways, finish)
    for step in range(1, nz):
        tok_forward(step, finish, nothing)
    for k in range(pieces):
        each_own(lambda way: w_copy(k, y, way, True), y, ny - 1, w_ways, finish)
        for step in range(1, ny):
            w_forward(k, step, finish, nothing)
    for j in range(1, n_ep):
        side_copy(j).wait_send()
    for q in range(chunks):
        for j in range(1, nx):
            for bz in range(nz):
                x_copy(q, j, bz).wait_send()
        for dz in range(nz):
            pl.when(z < dz)(lambda: r_copy(q, dz).wait_send())
            pl.when(z > dz)(lambda: l_copy(q, dz).wait_send())


def body(
    nx,
    nc,
    tokens,
    norm_gain,
    expert_ids,
    route_weights,
    expert_gate,
    expert_up,
    expert_down,
    shared_gate,
    shared_up,
    shared_down,
    side_in,
    side_out,
    side_gate,
):
    normed = normalize(tokens, norm_gain)
    tok_count, width = normed.shape
    n_ep, n_tp = lax.axis_size("ep"), lax.axis_size("tp")
    nz, ny = n_ep // nx, n_tp // nc
    me = lax.axis_index("ep")
    local_experts, ff_part, _ = expert_gate.shape
    experts_all = n_ep * local_experts
    shared_rows = shared_gate.shape[0] // n_ep
    side_rows, side_all = side_in.shape
    side_cols = side_all // n_ep
    chunks = 4
    piece = width // chunks

    named = expert_ids[:, :, None] == jnp.arange(experts_all, dtype=jnp.int32)
    dense = jnp.sum(jnp.where(named, route_weights[:, :, None], 0.0), axis=1)
    opening = jax.nn.sigmoid(jnp.dot(normed, side_gate, preferred_element_type=jnp.float32))
    aux = jnp.concatenate([dense, opening[:, None]], axis=1)
    aux = jnp.pad(aux, ((0, 0), (0, 64 - aux.shape[1])))
    high = lax.reduce_precision(aux, 8, 7)
    payload = jnp.concatenate(
        [normed, high.astype(jnp.bfloat16), (aux - high).astype(jnp.bfloat16)], axis=1
    )

    used = local_experts * ff_part + shared_rows
    part = -(-used // 16) * 16

    def pack(expert_part, shared_part):
        own = lax.dynamic_slice_in_dim(shared_part, me * shared_rows, shared_rows, 0)
        own = jnp.pad(own, ((0, part - used), (0, 0)))
        return jnp.concatenate([expert_part.reshape(local_experts * ff_part, width), own], axis=0)

    both = jnp.stack([side_in, side_out]).reshape(2, side_rows, n_ep, side_cols)
    both = both.transpose(2, 0, 1, 3)
    place = jnp.arange(n_tp * part, dtype=jnp.int32) % part // ff_part
    place = jnp.minimum(place, local_experts)
    mask = (place[None, :] == jnp.arange(local_experts + 1)[:, None]).astype(jnp.float32)

    bf16, f32 = jnp.bfloat16, jnp.float32
    dma = pltpu.SemaphoreType.DMA
    dims = (nz, nx, ny, nc, experts_all, local_experts, chunks)
    return pl.pallas_call(
        functools.partial(kernel, dims),
        out_shape=jax.ShapeDtypeStruct((tok_count, width), bf16),
        in_specs=[pl.BlockSpec(memory_space=pltpu.VMEM)] * 6,
        out_specs=pl.BlockSpec(memory_space=pltpu.VMEM),
        scratch_shapes=[
            pltpu.VMEM((n_ep * tok_count, payload.shape[1]), bf16),
            pltpu.VMEM((n_tp, part, width), bf16),
            pltpu.VMEM((n_tp, part, width), bf16),
            pltpu.VMEM((n_tp, part, width), bf16),
            pltpu.VMEM((n_ep, 2, side_rows, side_cols), bf16),
            pltpu.VMEM((n_ep * tok_count, n_tp * part), bf16),
            pltpu.VMEM((n_ep * tok_count, side_cols), bf16),
            pltpu.VMEM((chunks, nz * tok_count, piece), f32),
            pltpu.VMEM((chunks, nx - 1, nz * tok_count, piece), bf16),
            pltpu.VMEM((chunks, nx - 1, nz * tok_count, piece), bf16),
            pltpu.VMEM((chunks, nz, tok_count, piece), bf16),
            pltpu.VMEM((chunks, nz + 1, tok_count, piece), bf16),
            dma((nz, 1 + nx)),
            dma((n_ep,)),
            dma((2 + chunks, ny, 1 + nc)),
            dma((2 + chunks, n_tp)),
            dma((n_ep,)),
            dma((n_ep,)),
            dma((chunks, nx - 1, nz)),
            dma((chunks, nx - 1, nz)),
            dma((chunks, nz)),
            dma((chunks, nz)),
            dma((chunks, nz)),
            dma((chunks, nz)),
        ],
        compiler_params=pltpu.CompilerParams(
            collective_id=0, has_side_effects=True, vmem_limit_bytes=63000 * 1024
        ),
        name="layer",
    )(payload, pack(expert_gate, shared_gate), pack(expert_up, shared_up),
      pack(expert_down, shared_down), both, mask)


def solution(mesh):
    devices = mesh.devices
    nx = len({d.coords[0] for d in devices[:, 0]})
    nc = len({d.core_on_chip for d in devices[0, :]})
    placed = (
        P(("ep", "tp"), None),
        P(),
        P(("ep", "tp"), None),
        P(("ep", "tp"), None),
        P("ep", "tp", None),
        P("ep", "tp", None),
        P("ep", "tp", None),
        P("tp", None),
        P("tp", None),
        P("tp", None),
        P("ep", None),
        P("ep", None),
        P(),
    )
    return jax.shard_map(
        functools.partial(body, nx, nc),
        mesh=mesh,
        in_specs=placed,
        out_specs=P(("ep", "tp"), None),
        check_vma=False,
    )
```

```python
import functools

import jax
import jax.numpy as jnp
import numpy as np
from jax import lax
from jax.experimental import pallas as pl
from jax.experimental.pallas import tpu as pltpu
from jax.sharding import PartitionSpec as P

norm_eps = 1.0
MESH = pl.DeviceIdType.MESH
NT = (((1,), (1,)), ((), ()))


def silu(v):
    return v / (1.0 + jnp.exp(-v))


def kernel(
    dims,
    tokens_ref, gain_ref, ids_ref, route_ref, side_gate_ref, mask_ref,
    gate_ref, up_ref, down_ref, s_gate_ref, s_up_ref, s_down_ref, side_in_ref, side_out_ref,
    out_ref,
    tok, wg, wu, wd, side, hidden, side_hid, acc, xs, xr, sent, got,
    tok_send, tok_recv, w_send, w_recv, side_send, side_recv, swap_send, swap_recv, local_sem,
    x_send, x_recv, r_send, r_recv, l_send, l_recv,
):
    nz, nx, ny, nc, experts_all, local_experts, chunks = dims
    n_ep, n_tp = nz * nx, ny * nc
    me, tp = lax.axis_index("ep"), lax.axis_index("tp")
    z, x = me // nx, me % nx
    y, c = tp // nc, tp % nc
    rows = tokens_ref.shape[0]
    width = out_ref.shape[1]
    routed = gate_ref.shape[0]
    part, side_cols = wg.shape[1], side.shape[2]
    extra = part - routed
    piece = width // chunks
    side_rows = side.shape[1]

    def cols(q):
        return pl.ds(pl.multiple_of(q * piece, piece), piece)

    barrier = pltpu.get_barrier_semaphore()
    for j in range(1, n_ep):
        pl.semaphore_signal(barrier, inc=1, device_id=((me + j) % n_ep, tp), device_id_type=MESH)
    for j in range(1, n_tp):
        pl.semaphore_signal(barrier, inc=1, device_id=(me, (tp + j) % n_tp), device_id_type=MESH)
    pl.semaphore_wait(barrier, n_ep + n_tp - 2)

    def tok_rows(bz, bx):
        return pl.ds(pl.multiple_of((bx * nz + bz) * rows, rows), rows)

    def tok_copy(bz, way):
        if way < 2:
            target = (me + nx if way == 0 else me - nx, tp)
        else:
            target = (z * nx + (x + way - 1) % nx, tp)
        return pltpu.make_async_remote_copy(
            src_ref=tok.at[tok_rows(bz, x)],
            dst_ref=tok.at[tok_rows(bz, x)],
            send_sem=tok_send.at[bz, way],
            recv_sem=tok_recv.at[x * nz + bz],
            device_id=target,
            device_id_type=MESH,
        )

    def tok_wait(bz, bx):
        pltpu.make_async_remote_copy(
            src_ref=tok.at[tok_rows(bz, bx)],
            dst_ref=tok.at[tok_rows(bz, bx)],
            send_sem=tok_send.at[0, 0],
            recv_sem=tok_recv.at[bx * nz + bz],
            device_id=(me, tp),
            device_id_type=MESH,
        ).wait_recv()

    def w_place(k, owner):
        if k == 0:
            return wg.at[owner]
        if k == 1:
            return wu.at[owner]
        return wd.at[owner, :, cols(k - 2)]

    def own_parts(ref, shared_ref, place, q=None):
        at = pl.ds(pl.multiple_of(me * extra, extra), extra)
        at = at if shared_ref.shape[0] > extra else pl.ds(0, extra)
        head, tail = pl.ds(0, routed), pl.ds(routed, extra)
        if q is None:
            return (ref, place.at[head]), (shared_ref.at[at], place.at[tail])
        return (ref.at[:, q], place.at[head, q]), (shared_ref.at[at, q], place.at[tail, q])

    def w_parts(k):
        if k == 0:
            return own_parts(gate_ref, s_gate_ref, wg.at[tp])
        if k == 1:
            return own_parts(up_ref, s_up_ref, wu.at[tp])
        return own_parts(down_ref, s_down_ref, wd.at[tp], cols(k - 2))

    def w_copy(k, by, way, refs=None):
        if way < 2:
            target = (me, tp + nc if way == 0 else tp - nc)
        else:
            target = (me, y * nc + (c + way - 1) % nc)
        owner = by * nc + c
        src, dst = (w_place(k, owner), w_place(k, owner)) if refs is None else refs
        return pltpu.make_async_remote_copy(
            src_ref=src,
            dst_ref=dst,
            send_sem=w_send.at[k, by, way],
            recv_sem=w_recv.at[k, owner],
            device_id=target,
            device_id_type=MESH,
        )

    def w_wait(k, owner):
        pltpu.make_async_remote_copy(
            src_ref=w_place(k, owner), dst_ref=w_place(k, owner), send_sem=w_send.at[0, 0, 0],
            recv_sem=w_recv.at[k, owner], device_id=(me, tp), device_id_type=MESH,
        ).wait_recv()

    def side_source(ref, to):
        if len(ref.shape) == 3:
            return ref.at[to]
        return ref.at[:, pl.ds(pl.multiple_of(to * side_cols, side_cols), side_cols)]

    def side_copy(j, p):
        to = (me + j) % n_ep
        return pltpu.make_async_remote_copy(
            src_ref=side_source((side_in_ref, side_out_ref)[p], to),
            dst_ref=side.at[p * n_ep + me],
            send_sem=side_send.at[j],
            recv_sem=side_recv.at[me],
            device_id=(to, tp),
            device_id_type=MESH,
        )

    def side_each(act):
        for p in range(nc):

            @pl.when(c == p)
            def _():
                for j in range(1, n_ep):
                    act(side_copy(j, p))

    def side_own(p):
        return pltpu.make_async_copy(
            side_source((side_in_ref, side_out_ref)[p], me), side.at[p * n_ep + me],
            local_sem.at[3],
        )

    def swap_copy():
        half = side.at[pl.ds(c * n_ep, n_ep)]
        return pltpu.make_async_remote_copy(
            src_ref=half, dst_ref=half, send_sem=swap_send, recv_sem=swap_recv,
            device_id=(me, y * nc + 1 - c), device_id_type=MESH,
        )

    def each_own(copy_of, at, last, ways, act):
        @pl.when(at < last)
        def _():
            act(copy_of(0))

        @pl.when(at > 0)
        def _():
            act(copy_of(1))

        for way in range(2, ways):
            act(copy_of(way))

    def each_forward(copy_of, index_of, at, last, ways, step, act, arrive):
        @pl.when(at >= step)
        def _():
            b = at - step
            arrive(b)

            @pl.when(at < last)
            def _():
                act(copy_of(b, 0))

            for way in range(2, ways):
                act(copy_of(b, way))

        @pl.when(at + step <= last)
        def _():
            b = at + step
            arrive(b)

            @pl.when(at > 0)
            def _():
                act(copy_of(b, 1))

            for way in range(2, ways):
                act(copy_of(b, way))

    start = lambda copy: copy.start()
    finish = lambda copy: copy.wait_send()
    nothing = lambda b: None
    tok_ways, w_ways = 1 + nx, 1 + nc
    pieces = 2 + chunks

    def tok_forward(step, act, arrive):
        each_forward(
            lambda b, way: tok_copy(b, way), None, z, nz - 1, tok_ways, step, act, arrive
        )

    def w_forward(k, step, act, arrive):
        each_forward(
            lambda b, way: w_copy(k, b, way), None, y, ny - 1, w_ways, step, act, arrive
        )

    def w_gathered(k):
        for step in range(1, ny):
            w_forward(k, step, start, lambda b: w_wait(k, b * nc + c))

    def w_across(k):
        for j in range(1, nc):
            for by in range(ny):
                w_wait(k, by * nc + (c + j) % nc)

    for k in range(pieces):
        for refs in w_parts(k):
            each_own(lambda way: w_copy(k, y, way, refs), y, ny - 1, w_ways, start)
    whole_down = own_parts(down_ref, s_down_ref, wd.at[tp])
    for n, parts in enumerate((w_parts(0), w_parts(1), whole_down)):
        for src, dst in parts:
            pltpu.make_async_copy(src, dst, local_sem.at[n]).start()

    for p in range(nc):
        pl.when(c == p)(lambda: side_own(p).start())

    values = tokens_ref[...].astype(jnp.float32)
    scale_inv = lax.rsqrt(jnp.mean(values * values, axis=-1, keepdims=True) + norm_eps)
    normed = (values * scale_inv * gain_ref[...]).astype(jnp.bfloat16)
    mine = tok_rows(z, x)
    tok[mine, :width] = normed
    gated = normed.astype(jnp.float32) * side_gate_ref[...].astype(jnp.float32)
    opening = 1.0 / (1.0 + jnp.exp(-jnp.sum(gated, axis=-1, keepdims=True)))
    lane = lax.broadcasted_iota(jnp.int32, (rows, 128), 1)
    first = lane % 64
    aux = jnp.where(first == experts_all, opening, 0.0)
    for k in range(ids_ref.shape[1]):
        aux = aux + jnp.where(first == ids_ref[:, k : k + 1], route_ref[:, k : k + 1], 0.0)
    high = aux.astype(jnp.bfloat16)
    low = (aux - high.astype(jnp.float32)).astype(jnp.bfloat16)
    tok[mine, width:] = jnp.where(
        lane < 64, high.astype(jnp.float32), low.astype(jnp.float32)
    ).astype(jnp.bfloat16)
    each_own(lambda way: tok_copy(z, way), z, nz - 1, tok_ways, start)

    def arrive_tok(b):
        tok_wait(b, x)

    for step in range(1, nz):
        tok_forward(step, start, arrive_tok)
        if step == 1:
            side_each(start)
        if step == nz - 2:
            w_gathered(0)
    w_gathered(1)
    w_across(0)
    w_across(1)
    for n, place in enumerate((wg, wu, wd)):
        pltpu.make_async_copy(place.at[tp], place.at[tp], local_sem.at[n]).wait()

    tile = 2 * rows

    def column(at, n):
        aux = tok[at, width:].astype(jnp.float32)
        lane = lax.broadcasted_iota(jnp.int32, aux.shape, 1)
        hit = jnp.logical_or(lane == n, lane == n + 64)
        return jnp.sum(jnp.where(hit, aux, 0.0), axis=1, keepdims=True)

    for j in range(nx):
        bx = (x + j) % nx
        if j:
            for bz in range(nz):
                tok_wait(bz, bx)

        def hidden_tile(i, carry):
            at = pl.ds(pl.multiple_of(bx * nz * rows + i * tile, rows), tile)
            a = tok[at, :width]
            gate_part = lax.dot_general(
                a, wg[...].reshape(n_tp * part, width), NT, preferred_element_type=jnp.float32
            )
            up_part = lax.dot_general(
                a, wu[...].reshape(n_tp * part, width), NT, preferred_element_type=jnp.float32
            )
            scale = mask_ref[local_experts : local_experts + 1, :]
            for e in range(local_experts):
                scale = scale + column(at, me * local_experts + e) * mask_ref[e : e + 1, :]
            hidden[at] = (silu(gate_part) * up_part * scale).astype(jnp.bfloat16)
            return carry

        lax.fori_loop(0, nz * rows // tile, hidden_tile, 0)
        if j == 0:
            for p in range(nc):
                pl.when(c == p)(lambda: side_own(p).wait())
            for d in range(1, n_ep):
                at = (me + d) % n_ep
                block = side.at[c * n_ep + at]
                pltpu.make_async_remote_copy(
                    src_ref=block, dst_ref=block, send_sem=side_send.at[0],
                    recv_sem=side_recv.at[at], device_id=(me, tp), device_id_type=MESH,
                ).wait_recv()
            swap_copy().start()

    other = side.at[pl.ds((1 - c) * n_ep, n_ep)]
    pltpu.make_async_remote_copy(
        src_ref=other, dst_ref=other, send_sem=swap_send, recv_sem=swap_recv,
        device_id=(me, tp), device_id_type=MESH,
    ).wait_recv()

    def side_tile(i, carry):
        at = pl.ds(pl.multiple_of(i * tile, rows), tile)
        side_part = jnp.dot(
            tok[at, :width], side[:n_ep].reshape(width, side_cols),
            preferred_element_type=jnp.float32,
        )
        side_hid[at] = (silu(side_part) * column(at, experts_all)).astype(jnp.bfloat16)
        return carry

    lax.fori_loop(0, n_ep * rows // tile, side_tile, 0)

    def x_copy(q, j, bz):
        block = pl.ds(pl.multiple_of(bz * rows, rows), rows)
        return pltpu.make_async_remote_copy(
            src_ref=xs.at[q, j - 1, block],
            dst_ref=xr.at[q, j - 1, block],
            send_sem=x_send.at[q, j - 1, bz],
            recv_sem=x_recv.at[q, j - 1, bz],
            device_id=(z * nx + (x + j) % nx, tp),
            device_id_type=MESH,
        )

    def r_copy(q, dz):
        return pltpu.make_async_remote_copy(
            src_ref=sent.at[q, dz], dst_ref=got.at[q, dz + 1], send_sem=r_send.at[q, dz],
            recv_sem=r_recv.at[q, dz], device_id=(me + nx, tp), device_id_type=MESH,
        )

    def l_copy(q, dz):
        return pltpu.make_async_remote_copy(
            src_ref=sent.at[q, dz], dst_ref=got.at[q, dz], send_sem=l_send.at[q, dz],
            recv_sem=l_recv.at[q, dz], device_id=(me - nx, tp), device_id_type=MESH,
        )

    blocks_per = piece // side_rows

    def multiply(q):
        down = wd[:, :, cols(q)].reshape(n_tp * part, piece)
        side_down = side[pl.ds(n_ep + q * blocks_per, blocks_per)].reshape(piece, side_cols)
        for j in list(range(1, nx)) + [0]:
            at = pl.ds(pl.multiple_of((x + j) % nx * nz * rows, rows), nz * rows)
            value = jnp.dot(hidden[at], down, preferred_element_type=jnp.float32)
            value = value + lax.dot_general(
                side_hid[at], side_down, NT, preferred_element_type=jnp.float32
            )
            if j:
                xs[q, j - 1] = value.astype(jnp.bfloat16)
                for k in range(nz):
                    far = (1 - z * 2 // nz) * (nz - 1 - k) + z * 2 // nz * k
                    x_copy(q, j, far).start()
            else:
                acc[q] = value

    def reduce(q):
        def own(dz):
            block = pl.ds(pl.multiple_of(dz * rows, rows), rows)
            value = acc[q, block]
            for j in range(1, nx):
                x_copy(q, j, dz).wait_recv()
                value = value + xr[q, j - 1, block].astype(jnp.float32)
            return value

        def right(dz):
            value = own(dz)

            @pl.when(z == 0)
            def _():
                sent[q, dz] = value.astype(jnp.bfloat16)

            @pl.when(z > 0)
            def _():
                r_copy(q, dz).wait_recv()
                sent[q, dz] = (value + got[q, dz + 1].astype(jnp.float32)).astype(jnp.bfloat16)

            r_copy(q, dz).start()

        def left(dz):
            value = own(dz)

            @pl.when(z == nz - 1)
            def _():
                sent[q, dz] = value.astype(jnp.bfloat16)

            @pl.when(z < nz - 1)
            def _():
                l_copy(q, dz).wait_recv()
                sent[q, dz] = (value + got[q, dz].astype(jnp.float32)).astype(jnp.bfloat16)

            l_copy(q, dz).start()

        @pl.when(z * 2 < nz)
        def _():
            for k in range(nz - 1):
                pl.when(z < nz - 1 - k)(functools.partial(right, nz - 1 - k))
                pl.when(z > k)(functools.partial(left, k))

        @pl.when(z * 2 >= nz)
        def _():
            for k in range(nz - 1):
                pl.when(z > k)(functools.partial(left, k))
                pl.when(z < nz - 1 - k)(functools.partial(right, nz - 1 - k))

        acc[q, pl.ds(0, rows)] = own(z)

    def settle(q):
        @pl.when(z > 0)
        def _():
            r_copy(q, z).wait_recv()
            acc[q, pl.ds(0, rows)] += got[q, z + 1].astype(jnp.float32)

        @pl.when(z < nz - 1)
        def _():
            l_copy(q, z).wait_recv()
            acc[q, pl.ds(0, rows)] += got[q, z].astype(jnp.float32)

        out_ref[:, cols(q)] = acc[q, pl.ds(0, rows)].astype(jnp.bfloat16)

    for q in range(chunks):
        w_gathered(2 + q)
        w_across(2 + q)
        multiply(q)
        if q:
            reduce(q - 1)
    reduce(chunks - 1)
    for q in range(chunks):
        settle(q)

    each_own(lambda way: tok_copy(z, way), z, nz - 1, tok_ways, finish)
    for step in range(1, nz):
        tok_forward(step, finish, nothing)
    for k in range(pieces):
        each_own(lambda way: w_copy(k, y, way), y, ny - 1, w_ways, finish)
        for step in range(1, ny):
            w_forward(k, step, finish, nothing)
    side_each(finish)
    swap_copy().wait_send()
    for q in range(chunks):
        for j in range(1, nx):
            for bz in range(nz):
                x_copy(q, j, bz).wait_send()
        for dz in range(nz):
            pl.when(z < dz)(lambda: r_copy(q, dz).wait_send())
            pl.when(z > dz)(lambda: l_copy(q, dz).wait_send())


def body(
    nx,
    nc,
    tokens,
    norm_gain,
    expert_ids,
    route_weights,
    expert_gate,
    expert_up,
    expert_down,
    shared_gate,
    shared_up,
    shared_down,
    side_in,
    side_out,
    side_gate,
):
    tok_count, width = tokens.shape
    n_ep, n_tp = lax.axis_size("ep"), lax.axis_size("tp")
    nz, ny = n_ep // nx, n_tp // nc
    me = lax.axis_index("ep")
    local_experts, ff_part, _ = expert_gate.shape
    routed = local_experts * ff_part
    experts_all = n_ep * local_experts
    shared_rows = shared_gate.shape[0] // n_ep
    side_rows, side_all = side_in.shape
    side_cols = side_all // n_ep
    chunks = 8
    piece = width // chunks
    part = routed + -(-shared_rows // 16) * 16

    def shared_part(array):
        if shared_rows % 16 == 0:
            return array
        own = lax.dynamic_slice_in_dim(array, me * shared_rows, shared_rows, 0)
        return jnp.pad(own, ((0, part - routed - shared_rows), (0, 0)))

    def side_part(array):
        if side_cols % 128 == 0:
            return array
        return array.reshape(side_rows, n_ep, side_cols).transpose(1, 0, 2)

    place = np.minimum(np.arange(n_tp * part) % part // ff_part, local_experts)
    mask = (place[None, :] == np.arange(local_experts + 1)[:, None]).astype(np.float32)

    bf16, f32 = jnp.bfloat16, jnp.float32
    dma = pltpu.SemaphoreType.DMA
    dims = (nz, nx, ny, nc, experts_all, local_experts, chunks)
    return pl.pallas_call(
        functools.partial(kernel, dims),
        out_shape=jax.ShapeDtypeStruct((tok_count, width), bf16),
        in_specs=[pl.BlockSpec(memory_space=pltpu.VMEM)] * 6
        + [pl.BlockSpec(memory_space=pl.ANY)] * 8,
        out_specs=pl.BlockSpec(memory_space=pltpu.VMEM),
        scratch_shapes=[
            pltpu.VMEM((n_ep * tok_count, width + 128), bf16),
            pltpu.VMEM((n_tp, part, width), bf16),
            pltpu.VMEM((n_tp, part, width), bf16),
            pltpu.VMEM((n_tp, part, width), bf16),
            pltpu.VMEM((2 * n_ep, side_rows, side_cols), bf16),
            pltpu.VMEM((n_ep * tok_count, n_tp * part), bf16),
            pltpu.VMEM((n_ep * tok_count, side_cols), bf16),
            pltpu.VMEM((chunks, nz * tok_count, piece), f32),
            pltpu.VMEM((chunks, nx - 1, nz * tok_count, piece), bf16),
            pltpu.VMEM((chunks, nx - 1, nz * tok_count, piece), bf16),
            pltpu.VMEM((chunks, nz, tok_count, piece), bf16),
            pltpu.VMEM((chunks, nz + 1, tok_count, piece), bf16),
            dma((nz, 1 + nx)),
            dma((n_ep,)),
            dma((2 + chunks, ny, 1 + nc)),
            dma((2 + chunks, n_tp)),
            dma((n_ep,)),
            dma((n_ep,)),
            dma,
            dma,
            dma((4,)),
            dma((chunks, nx - 1, nz)),
            dma((chunks, nx - 1, nz)),
            dma((chunks, nz)),
            dma((chunks, nz)),
            dma((chunks, nz)),
            dma((chunks, nz)),
        ],
        compiler_params=pltpu.CompilerParams(
            collective_id=0, has_side_effects=True, vmem_limit_bytes=63000 * 1024
        ),
        name="layer",
    )(
        tokens, norm_gain[None, :], expert_ids, route_weights, side_gate[None, :], mask,
        expert_gate.reshape(routed, width), expert_up.reshape(routed, width),
        expert_down.reshape(routed, width), shared_part(shared_gate), shared_part(shared_up),
        shared_part(shared_down), side_part(side_in), side_part(side_out),
    )


def solution(mesh):
    devices = mesh.devices
    nx = len({d.coords[0] for d in devices[:, 0]})
    nc = len({d.core_on_chip for d in devices[0, :]})
    placed = (
        P(("ep", "tp"), None),
        P(),
        P(("ep", "tp"), None),
        P(("ep", "tp"), None),
        P("ep", "tp", None),
        P("ep", "tp", None),
        P("ep", "tp", None),
        P("tp", None),
        P("tp", None),
        P("tp", None),
        P("ep", None),
        P("ep", None),
        P(),
    )
    return jax.shard_map(
        functools.partial(body, nx, nc),
        mesh=mesh,
        in_specs=placed,
        out_specs=P(("ep", "tp"), None),
        check_vma=False,
    )
```

```python
import functools

import jax
import jax.numpy as jnp
import numpy as np
from jax import lax
from jax.experimental import pallas as pl
from jax.experimental.pallas import tpu as pltpu
from jax.sharding import PartitionSpec as P

norm_eps = 1.0
MESH = pl.DeviceIdType.MESH
NT = (((1,), (1,)), ((), ()))


def silu(v):
    return v / (1.0 + jnp.exp(-v))


def kernel(
    dims,
    tokens_ref, gain_ref, ids_ref, route_ref, side_gate_ref, mask_ref,
    gate_ref, up_ref, down_ref, s_gate_ref, s_up_ref, s_down_ref, side_in_ref, side_out_ref,
    out_ref,
    tok, wg, wu, wd, side, hidden, side_hid, acc, xs, xr, sent, got,
    tok_send, tok_recv, w_send, w_recv, side_send, side_recv, swap_send, swap_recv, local_sem,
    x_send, x_recv, r_send, r_recv, l_send, l_recv,
):
    nz, nx, ny, nc, experts_all, local_experts, chunks = dims
    n_ep, n_tp = nz * nx, ny * nc
    me, tp = lax.axis_index("ep"), lax.axis_index("tp")
    z, x = me // nx, me % nx
    y, c = tp // nc, tp % nc
    rows = tokens_ref.shape[0]
    width = out_ref.shape[1]
    routed = gate_ref.shape[0]
    part, side_cols = wg.shape[1], side.shape[2]
    extra = part - routed
    piece = width // chunks
    side_rows = side.shape[1]

    def cols(q):
        return pl.ds(pl.multiple_of(q * piece, piece), piece)

    barrier = pltpu.get_barrier_semaphore()
    for j in range(1, n_ep):
        pl.semaphore_signal(barrier, inc=1, device_id=((me + j) % n_ep, tp), device_id_type=MESH)
    for j in range(1, n_tp):
        pl.semaphore_signal(barrier, inc=1, device_id=(me, (tp + j) % n_tp), device_id_type=MESH)
    pl.semaphore_wait(barrier, n_ep + n_tp - 2)

    def tok_rows(bz, bx):
        return pl.ds(pl.multiple_of((bx * nz + bz) * rows, rows), rows)

    def tok_copy(bz, way):
        if way < 2:
            target = (me + nx if way == 0 else me - nx, tp)
        else:
            target = (z * nx + (x + way - 1) % nx, tp)
        return pltpu.make_async_remote_copy(
            src_ref=tok.at[tok_rows(bz, x)],
            dst_ref=tok.at[tok_rows(bz, x)],
            send_sem=tok_send.at[bz, way],
            recv_sem=tok_recv.at[x * nz + bz],
            device_id=target,
            device_id_type=MESH,
        )

    def tok_wait(bz, bx):
        pltpu.make_async_remote_copy(
            src_ref=tok.at[tok_rows(bz, bx)],
            dst_ref=tok.at[tok_rows(bz, bx)],
            send_sem=tok_send.at[0, 0],
            recv_sem=tok_recv.at[bx * nz + bz],
            device_id=(me, tp),
            device_id_type=MESH,
        ).wait_recv()

    def w_place(k, owner):
        if k == 0:
            return wg.at[owner]
        if k == 1:
            return wu.at[owner]
        return wd.at[owner, :, cols(k - 2)]

    def own_parts(ref, shared_ref, place, q=None):
        at = pl.ds(pl.multiple_of(me * extra, extra), extra)
        at = at if shared_ref.shape[0] > extra else pl.ds(0, extra)
        head, tail = pl.ds(0, routed), pl.ds(routed, extra)
        if q is None:
            return (ref, place.at[head]), (shared_ref.at[at], place.at[tail])
        return (ref.at[:, q], place.at[head, q]), (shared_ref.at[at, q], place.at[tail, q])

    def w_parts(k):
        if k == 0:
            return own_parts(gate_ref, s_gate_ref, wg.at[tp])
        if k == 1:
            return own_parts(up_ref, s_up_ref, wu.at[tp])
        return own_parts(down_ref, s_down_ref, wd.at[tp], cols(k - 2))

    def w_copy(k, by, way, refs=None):
        if way < 2:
            target = (me, tp + nc if way == 0 else tp - nc)
        else:
            target = (me, y * nc + (c + way - 1) % nc)
        owner = by * nc + c
        src, dst = (w_place(k, owner), w_place(k, owner)) if refs is None else refs
        return pltpu.make_async_remote_copy(
            src_ref=src,
            dst_ref=dst,
            send_sem=w_send.at[k, by, way],
            recv_sem=w_recv.at[k, owner],
            device_id=target,
            device_id_type=MESH,
        )

    def w_wait(k, owner):
        pltpu.make_async_remote_copy(
            src_ref=w_place(k, owner), dst_ref=w_place(k, owner), send_sem=w_send.at[0, 0, 0],
            recv_sem=w_recv.at[k, owner], device_id=(me, tp), device_id_type=MESH,
        ).wait_recv()

    def side_source(ref, to):
        if len(ref.shape) == 3:
            return ref.at[to]
        return ref.at[:, pl.ds(pl.multiple_of(to * side_cols, side_cols), side_cols)]

    def side_copy(j, p):
        to = (me + j) % n_ep
        return pltpu.make_async_remote_copy(
            src_ref=side_source((side_in_ref, side_out_ref)[p], to),
            dst_ref=side.at[p * n_ep + me],
            send_sem=side_send.at[j],
            recv_sem=side_recv.at[me],
            device_id=(to, tp),
            device_id_type=MESH,
        )

    def side_each(act):
        for p in range(nc):

            @pl.when(c == p)
            def _():
                for j in range(1, n_ep):
                    act(side_copy(j, p))

    def side_own(p):
        return pltpu.make_async_copy(
            side_source((side_in_ref, side_out_ref)[p], me), side.at[p * n_ep + me],
            local_sem.at[3],
        )

    def swap_copy():
        half = side.at[pl.ds(c * n_ep, n_ep)]
        return pltpu.make_async_remote_copy(
            src_ref=half, dst_ref=half, send_sem=swap_send, recv_sem=swap_recv,
            device_id=(me, y * nc + 1 - c), device_id_type=MESH,
        )

    def each_own(copy_of, at, last, ways, act):
        @pl.when(at < last)
        def _():
            act(copy_of(0))

        @pl.when(at > 0)
        def _():
            act(copy_of(1))

        for way in range(2, ways):
            act(copy_of(way))

    def each_forward(copy_of, index_of, at, last, ways, step, act, arrive):
        @pl.when(at >= step)
        def _():
            b = at - step
            arrive(b)

            @pl.when(at < last)
            def _():
                act(copy_of(b, 0))

            for way in range(2, ways):
                act(copy_of(b, way))

        @pl.when(at + step <= last)
        def _():
            b = at + step
            arrive(b)

            @pl.when(at > 0)
            def _():
                act(copy_of(b, 1))

            for way in range(2, ways):
                act(copy_of(b, way))

    start = lambda copy: copy.start()
    finish = lambda copy: copy.wait_send()
    nothing = lambda b: None
    tok_ways, w_ways = 1 + nx, 1 + nc
    pieces = 2 + chunks

    def tok_forward(step, act, arrive):
        each_forward(
            lambda b, way: tok_copy(b, way), None, z, nz - 1, tok_ways, step, act, arrive
        )

    def w_forward(k, step, act, arrive):
        each_forward(
            lambda b, way: w_copy(k, b, way), None, y, ny - 1, w_ways, step, act, arrive
        )

    def w_gathered(k):
        for step in range(1, ny):
            w_forward(k, step, start, lambda b: w_wait(k, b * nc + c))

    def w_across(k):
        for j in range(1, nc):
            for by in range(ny):
                w_wait(k, by * nc + (c + j) % nc)

    for k in range(pieces):
        for refs in w_parts(k):
            each_own(lambda way: w_copy(k, y, way, refs), y, ny - 1, w_ways, start)
    whole_down = own_parts(down_ref, s_down_ref, wd.at[tp])
    for n, parts in enumerate((w_parts(0), w_parts(1), whole_down)):
        for src, dst in parts:
            pltpu.make_async_copy(src, dst, local_sem.at[n]).start()

    for p in range(nc):
        pl.when(c == p)(lambda: side_own(p).start())

    values = tokens_ref[...].astype(jnp.float32)
    scale_inv = lax.rsqrt(jnp.mean(values * values, axis=-1, keepdims=True) + norm_eps)
    normed = (values * scale_inv * gain_ref[...]).astype(jnp.bfloat16)
    mine = tok_rows(z, x)
    tok[mine, :width] = normed
    gated = normed.astype(jnp.float32) * side_gate_ref[...].astype(jnp.float32)
    opening = 1.0 / (1.0 + jnp.exp(-jnp.sum(gated, axis=-1, keepdims=True)))
    lane = lax.broadcasted_iota(jnp.int32, (rows, 128), 1)
    first = lane % 64
    aux = jnp.where(first == experts_all, opening, 0.0)
    for k in range(ids_ref.shape[1]):
        aux = aux + jnp.where(first == ids_ref[:, k : k + 1], route_ref[:, k : k + 1], 0.0)
    high = aux.astype(jnp.bfloat16)
    low = (aux - high.astype(jnp.float32)).astype(jnp.bfloat16)
    tok[mine, width:] = jnp.where(
        lane < 64, high.astype(jnp.float32), low.astype(jnp.float32)
    ).astype(jnp.bfloat16)
    each_own(lambda way: tok_copy(z, way), z, nz - 1, tok_ways, start)

    def arrive_tok(b):
        tok_wait(b, x)

    for step in range(1, nz):
        tok_forward(step, start, arrive_tok)
        if step == 1:
            side_each(start)
        if step == nz - 2:
            w_gathered(0)
    w_gathered(1)
    w_across(0)
    w_across(1)
    for n, place in enumerate((wg, wu, wd)):
        pltpu.make_async_copy(place.at[tp], place.at[tp], local_sem.at[n]).wait()

    tile = 2 * rows

    def column(at, n):
        aux = tok[at, width:].astype(jnp.float32)
        lane = lax.broadcasted_iota(jnp.int32, aux.shape, 1)
        hit = jnp.logical_or(lane == n, lane == n + 64)
        return jnp.sum(jnp.where(hit, aux, 0.0), axis=1, keepdims=True)

    for j in range(nx):
        bx = (x + j) % nx

        def hidden_tile(i, carry):
            pair = (z // 2 + i) % (nz // 2)
            if j:
                tok_wait(2 * pair, bx)
                tok_wait(2 * pair + 1, bx)
            at = pl.ds(pl.multiple_of(bx * nz * rows + pair * tile, rows), tile)
            a = tok[at, :width]
            gate_part = lax.dot_general(
                a, wg[...].reshape(n_tp * part, width), NT, preferred_element_type=jnp.float32
            )
            up_part = lax.dot_general(
                a, wu[...].reshape(n_tp * part, width), NT, preferred_element_type=jnp.float32
            )
            scale = mask_ref[local_experts : local_experts + 1, :]
            for e in range(local_experts):
                scale = scale + column(at, me * local_experts + e) * mask_ref[e : e + 1, :]
            hidden[at] = (silu(gate_part) * up_part * scale).astype(jnp.bfloat16)
            return carry

        lax.fori_loop(0, nz // 2, hidden_tile, 0)
        if j == 0:
            for p in range(nc):
                pl.when(c == p)(lambda: side_own(p).wait())
            for d in range(1, n_ep):
                at = (me + d) % n_ep
                block = side.at[c * n_ep + at]
                pltpu.make_async_remote_copy(
                    src_ref=block, dst_ref=block, send_sem=side_send.at[0],
                    recv_sem=side_recv.at[at], device_id=(me, tp), device_id_type=MESH,
                ).wait_recv()
            swap_copy().start()

    other = side.at[pl.ds((1 - c) * n_ep, n_ep)]
    pltpu.make_async_remote_copy(
        src_ref=other, dst_ref=other, send_sem=swap_send, recv_sem=swap_recv,
        device_id=(me, tp), device_id_type=MESH,
    ).wait_recv()

    def side_tile(i, carry):
        at = pl.ds(pl.multiple_of(i * tile, rows), tile)
        side_part = jnp.dot(
            tok[at, :width], side[:n_ep].reshape(width, side_cols),
            preferred_element_type=jnp.float32,
        )
        side_hid[at] = (silu(side_part) * column(at, experts_all)).astype(jnp.bfloat16)
        return carry

    lax.fori_loop(0, n_ep * rows // tile, side_tile, 0)

    def x_copy(q, j, bz):
        block = pl.ds(pl.multiple_of(bz * rows, rows), rows)
        return pltpu.make_async_remote_copy(
            src_ref=xs.at[q, j - 1, block],
            dst_ref=xr.at[q, j - 1, block],
            send_sem=x_send.at[q, j - 1, bz],
            recv_sem=x_recv.at[q, j - 1, bz],
            device_id=(z * nx + (x + j) % nx, tp),
            device_id_type=MESH,
        )

    def r_copy(q, dz):
        return pltpu.make_async_remote_copy(
            src_ref=sent.at[q, dz], dst_ref=got.at[q, dz + 1], send_sem=r_send.at[q, dz],
            recv_sem=r_recv.at[q, dz], device_id=(me + nx, tp), device_id_type=MESH,
        )

    def l_copy(q, dz):
        return pltpu.make_async_remote_copy(
            src_ref=sent.at[q, dz], dst_ref=got.at[q, dz], send_sem=l_send.at[q, dz],
            recv_sem=l_recv.at[q, dz], device_id=(me - nx, tp), device_id_type=MESH,
        )

    blocks_per = piece // side_rows

    def multiply(q):
        down = wd[:, :, cols(q)].reshape(n_tp * part, piece)
        side_down = side[pl.ds(n_ep + q * blocks_per, blocks_per)].reshape(piece, side_cols)
        for j in list(range(1, nx)) + [0]:
            at = pl.ds(pl.multiple_of((x + j) % nx * nz * rows, rows), nz * rows)
            value = jnp.dot(hidden[at], down, preferred_element_type=jnp.float32)
            value = value + lax.dot_general(
                side_hid[at], side_down, NT, preferred_element_type=jnp.float32
            )
            if j:
                xs[q, j - 1] = value.astype(jnp.bfloat16)
                for k in range(nz):
                    far = (1 - z * 2 // nz) * (nz - 1 - k) + z * 2 // nz * k
                    x_copy(q, j, far).start()
            else:
                acc[q] = value

    def reduce(q):
        def own(dz):
            block = pl.ds(pl.multiple_of(dz * rows, rows), rows)
            value = acc[q, block]
            for j in range(1, nx):
                x_copy(q, j, dz).wait_recv()
                value = value + xr[q, j - 1, block].astype(jnp.float32)
            return value

        def right(dz):
            value = own(dz)

            @pl.when(z == 0)
            def _():
                sent[q, dz] = value.astype(jnp.bfloat16)

            @pl.when(z > 0)
            def _():
                r_copy(q, dz).wait_recv()
                sent[q, dz] = (value + got[q, dz + 1].astype(jnp.float32)).astype(jnp.bfloat16)

            r_copy(q, dz).start()

        def left(dz):
            value = own(dz)

            @pl.when(z == nz - 1)
            def _():
                sent[q, dz] = value.astype(jnp.bfloat16)

            @pl.when(z < nz - 1)
            def _():
                l_copy(q, dz).wait_recv()
                sent[q, dz] = (value + got[q, dz].astype(jnp.float32)).astype(jnp.bfloat16)

            l_copy(q, dz).start()

        @pl.when(z * 2 < nz)
        def _():
            for k in range(nz - 1):
                pl.when(z < nz - 1 - k)(functools.partial(right, nz - 1 - k))
                pl.when(z > k)(functools.partial(left, k))

        @pl.when(z * 2 >= nz)
        def _():
            for k in range(nz - 1):
                pl.when(z > k)(functools.partial(left, k))
                pl.when(z < nz - 1 - k)(functools.partial(right, nz - 1 - k))

        acc[q, pl.ds(0, rows)] = own(z)

    def settle(q):
        @pl.when(z > 0)
        def _():
            r_copy(q, z).wait_recv()
            acc[q, pl.ds(0, rows)] += got[q, z + 1].astype(jnp.float32)

        @pl.when(z < nz - 1)
        def _():
            l_copy(q, z).wait_recv()
            acc[q, pl.ds(0, rows)] += got[q, z].astype(jnp.float32)

        out_ref[:, cols(q)] = acc[q, pl.ds(0, rows)].astype(jnp.bfloat16)

    for q in range(chunks):
        w_gathered(2 + q)
        w_across(2 + q)
        multiply(q)
        if q:
            reduce(q - 1)
    reduce(chunks - 1)
    for q in range(chunks):
        settle(q)

    each_own(lambda way: tok_copy(z, way), z, nz - 1, tok_ways, finish)
    for step in range(1, nz):
        tok_forward(step, finish, nothing)
    for k in range(pieces):
        each_own(lambda way: w_copy(k, y, way), y, ny - 1, w_ways, finish)
        for step in range(1, ny):
            w_forward(k, step, finish, nothing)
    side_each(finish)
    swap_copy().wait_send()
    for q in range(chunks):
        for j in range(1, nx):
            for bz in range(nz):
                x_copy(q, j, bz).wait_send()
        for dz in range(nz):
            pl.when(z < dz)(lambda: r_copy(q, dz).wait_send())
            pl.when(z > dz)(lambda: l_copy(q, dz).wait_send())


def body(
    nx,
    nc,
    tokens,
    norm_gain,
    expert_ids,
    route_weights,
    expert_gate,
    expert_up,
    expert_down,
    shared_gate,
    shared_up,
    shared_down,
    side_in,
    side_out,
    side_gate,
):
    tok_count, width = tokens.shape
    n_ep, n_tp = lax.axis_size("ep"), lax.axis_size("tp")
    nz, ny = n_ep // nx, n_tp // nc
    me = lax.axis_index("ep")
    local_experts, ff_part, _ = expert_gate.shape
    routed = local_experts * ff_part
    experts_all = n_ep * local_experts
    shared_rows = shared_gate.shape[0] // n_ep
    side_rows, side_all = side_in.shape
    side_cols = side_all // n_ep
    chunks = 8
    piece = width // chunks
    part = routed + -(-shared_rows // 16) * 16

    def shared_part(array):
        if shared_rows % 16 == 0:
            return array
        own = lax.dynamic_slice_in_dim(array, me * shared_rows, shared_rows, 0)
        return jnp.pad(own, ((0, part - routed - shared_rows), (0, 0)))

    def side_part(array):
        if side_cols % 128 == 0:
            return array
        return array.reshape(side_rows, n_ep, side_cols).transpose(1, 0, 2)

    place = np.minimum(np.arange(n_tp * part) % part // ff_part, local_experts)
    mask = (place[None, :] == np.arange(local_experts + 1)[:, None]).astype(np.float32)

    bf16, f32 = jnp.bfloat16, jnp.float32
    dma = pltpu.SemaphoreType.DMA
    dims = (nz, nx, ny, nc, experts_all, local_experts, chunks)
    return pl.pallas_call(
        functools.partial(kernel, dims),
        out_shape=jax.ShapeDtypeStruct((tok_count, width), bf16),
        in_specs=[pl.BlockSpec(memory_space=pltpu.VMEM)] * 6
        + [pl.BlockSpec(memory_space=pl.ANY)] * 8,
        out_specs=pl.BlockSpec(memory_space=pltpu.VMEM),
        scratch_shapes=[
            pltpu.VMEM((n_ep * tok_count, width + 128), bf16),
            pltpu.VMEM((n_tp, part, width), bf16),
            pltpu.VMEM((n_tp, part, width), bf16),
            pltpu.VMEM((n_tp, part, width), bf16),
            pltpu.VMEM((2 * n_ep, side_rows, side_cols), bf16),
            pltpu.VMEM((n_ep * tok_count, n_tp * part), bf16),
            pltpu.VMEM((n_ep * tok_count, side_cols), bf16),
            pltpu.VMEM((chunks, nz * tok_count, piece), f32),
            pltpu.VMEM((chunks, nx - 1, nz * tok_count, piece), bf16),
            pltpu.VMEM((chunks, nx - 1, nz * tok_count, piece), bf16),
            pltpu.VMEM((chunks, nz, tok_count, piece), bf16),
            pltpu.VMEM((chunks, nz + 1, tok_count, piece), bf16),
            dma((nz, 1 + nx)),
            dma((n_ep,)),
            dma((2 + chunks, ny, 1 + nc)),
            dma((2 + chunks, n_tp)),
            dma((n_ep,)),
            dma((n_ep,)),
            dma,
            dma,
            dma((4,)),
            dma((chunks, nx - 1, nz)),
            dma((chunks, nx - 1, nz)),
            dma((chunks, nz)),
            dma((chunks, nz)),
            dma((chunks, nz)),
            dma((chunks, nz)),
        ],
        compiler_params=pltpu.CompilerParams(
            collective_id=0, has_side_effects=True, vmem_limit_bytes=63000 * 1024
        ),
        name="layer",
    )(
        tokens, norm_gain[None, :], expert_ids, route_weights, side_gate[None, :], mask,
        expert_gate.reshape(routed, width), expert_up.reshape(routed, width),
        expert_down.reshape(routed, width), shared_part(shared_gate), shared_part(shared_up),
        shared_part(shared_down), side_part(side_in), side_part(side_out),
    )


def solution(mesh):
    devices = mesh.devices
    nx = len({d.coords[0] for d in devices[:, 0]})
    nc = len({d.core_on_chip for d in devices[0, :]})
    placed = (
        P(("ep", "tp"), None),
        P(),
        P(("ep", "tp"), None),
        P(("ep", "tp"), None),
        P("ep", "tp", None),
        P("ep", "tp", None),
        P("ep", "tp", None),
        P("tp", None),
        P("tp", None),
        P("tp", None),
        P("ep", None),
        P("ep", None),
        P(),
    )
    return jax.shard_map(
        functools.partial(body, nx, nc),
        mesh=mesh,
        in_specs=placed,
        out_specs=P(("ep", "tp"), None),
        check_vma=False,
    )
```
